32 devices in a mesh: sp: 8 (over z, y), tp: 4 (over x, core).
Axes of the slice: x: 2, y: 2, z: 4, core: 2. Of those that a mesh axis runs over, the one named last changes fastest.
Arguments:
- residual: bfloat16 [4096, 2048], P(('sp', 'tp')), may hold values from -6 to 6
- query_major: bfloat16 [4096, 1024], P('sp', 'tp'), may hold values from -160 to 160
- keys_major: bfloat16 [4096, 1024], P('sp', 'tp'), may hold values from -6.5 to 6.5
- values_major: bfloat16 [4096, 1024], P('sp', 'tp'), may hold values from -6 to 6
- query_minor: bfloat16 [4096, 512], P('sp', 'tp'), may hold values from -160 to 160
- keys_minor: bfloat16 [4096, 512], P('sp', 'tp'), may hold values from -6.5 to 6.5
- values_minor: bfloat16 [4096, 512], P('sp', 'tp'), may hold values from -6 to 6
- lambda_major: float32 [8], P('tp'), may hold values from 0.3 to 0.8
- lambda_minor: float32 [8], P('tp'), may hold values from 0.3 to 0.8
- gain_major: float32 [128], replicated, may hold values from 0.1 to 1.9
- gain_minor: float32 [64], replicated, may hold values from 0.1 to 1.9
- output_major: bfloat16 [1024, 2048], P('tp'), may hold values from -0.15625 to 0.15625
- output_minor: bfloat16 [512, 2048], P('tp'), may hold values from -0.15625 to 0.15625
- mixer_gain: float32 [2048], replicated, may hold values from 0.1 to 1.9
- up_weight: bfloat16 [2048, 8192], P('sp', 'tp'), may hold values from -0.125 to 0.125
- down_weight: bfloat16 [8192, 2048], P('tp', 'sp'), may hold values from -0.0625 to 0.0625
Outputs:
- layer_out: bfloat16 [4096, 2048], P(('sp', 'tp'))
The draws below stay inside these ranges and needn't reach their ends.
All inputs are finite; a program needn't handle non-finite values.
Results may differ from the reference program's by a relative error of at most 0.018.
Values may be sent and summed in bfloat16 or wider, within the bound.
A program may use at most 128 MiB of HBM per device.

```python
import jax
import jax.numpy as jnp
from jax import lax

D_MODEL = 2048
D_FF = 8192
H_MAJOR = 8
DK_MAJOR = 64
H_MINOR = 8
DK_MINOR = 32
DV_MAJOR = 128
DV_MINOR = 64
SEGMENT = 64
TOKENS = 4096
N_TP = 4


def drawn(key, head_count, key_size):
    key_query, key_keys = jax.random.split(key, 2)
    shape = (TOKENS, head_count, 2, key_size)
    queries = jnp.clip(jax.random.normal(key_query, shape, jnp.float32), -5.0, 5.0) * 1.3
    key_rows = jnp.clip(jax.random.normal(key_keys, shape, jnp.float32), -5.0, 5.0) * 1.3
    width_all = head_count * 2 * key_size
    return (queries.reshape(TOKENS, width_all), key_rows.reshape(TOKENS, width_all))


def draw_query_major(key, part):
    return drawn(jax.random.fold_in(key, 1), H_MAJOR, DK_MAJOR)[0].astype(jnp.bfloat16)


def draw_keys_major(key, part):
    return drawn(jax.random.fold_in(key, 1), H_MAJOR, DK_MAJOR)[1].astype(jnp.bfloat16)


def draw_query_minor(key, part):
    return drawn(jax.random.fold_in(key, 2), H_MINOR, DK_MINOR)[0].astype(jnp.bfloat16)


def draw_keys_minor(key, part):
    return drawn(jax.random.fold_in(key, 2), H_MINOR, DK_MINOR)[1].astype(jnp.bfloat16)


def shard_levels(stream_key, dims, cuts, low, high):
    gain, own = 1.0, jax.random.fold_in(stream_key, 6)
    for axis_at, blocks in cuts:
        draws = jnp.exp(jax.random.uniform(jax.random.fold_in(own, axis_at), (blocks,), jnp.float32, low / len(cuts), high / len(cuts)))
        gain = gain * jnp.repeat(draws, dims[axis_at] // blocks).reshape([-1 if axis == axis_at else 1 for axis in range(len(dims))])
    return gain


def normal_values(rng, dims, width, reach, shards=(), kind=jnp.bfloat16):
    gain = shard_levels(rng, dims, shards, -0.22, 0.18) if shards else 1.0
    result = jax.random.normal(rng, dims, jnp.float32) * width * gain
    return jnp.minimum(jnp.maximum(result, -reach), reach).astype(kind)


def setup_inputs(seed: int = 0) -> dict:
    keys = jax.random.split(jax.random.key(seed), 17)
    residual = normal_values(keys[0], (TOKENS, D_MODEL), 1.0, 6.0, ((0, 32),))
    query_major = draw_query_major(jax.random.fold_in(keys[16], 71), 0)
    keys_major = draw_keys_major(jax.random.fold_in(keys[16], 71), 0)
    values_major = normal_values(keys[3], (TOKENS, H_MAJOR * DV_MAJOR), 1.0, 6.0, ((0, 8), (1, 4)))
    query_minor = draw_query_minor(jax.random.fold_in(keys[16], 71), 0)
    keys_minor = draw_keys_minor(jax.random.fold_in(keys[16], 71), 0)
    values_minor = normal_values(keys[6], (TOKENS, H_MINOR * DV_MINOR), 1.0, 6.0, ((0, 8), (1, 4)))
    lambda_major = jnp.clip(0.3 + 0.5 * jax.random.uniform(keys[7], (H_MAJOR,), jnp.float32) ** shard_levels(keys[7], (H_MAJOR,), ((0, 4),), -0.2, 0.2), 0.3, 0.8)
    lambda_minor = jnp.clip(0.3 + 0.5 * jax.random.uniform(keys[8], (H_MINOR,), jnp.float32) ** shard_levels(keys[8], (H_MINOR,), ((0, 4),), -0.2, 0.2), 0.3, 0.8)
    gain_major = jnp.clip(1.0 + 0.18 * jax.random.normal(keys[9], (DV_MAJOR,), jnp.float32), 0.1, 1.9)
    gain_minor = jnp.clip(1.0 + 0.18 * jax.random.normal(keys[10], (DV_MINOR,), jnp.float32), 0.1, 1.9)
    output_major = normal_values(keys[11], (H_MAJOR * DV_MAJOR, D_MODEL), (H_MAJOR * DV_MAJOR + H_MINOR * DV_MINOR) ** -0.5, 0.15625, ((0, 4),))
    output_minor = normal_values(keys[12], (H_MINOR * DV_MINOR, D_MODEL), (H_MAJOR * DV_MAJOR + H_MINOR * DV_MINOR) ** -0.5, 0.15625, ((0, 4),))
    mixer_gain = jnp.clip(1.0 + 0.18 * jax.random.normal(keys[13], (D_MODEL,), jnp.float32), 0.1, 1.9)
    up_weight = normal_values(keys[14], (D_MODEL, D_FF), D_MODEL ** -0.5, 0.125, ((0, 8), (1, 4)))
    down_weight = normal_values(keys[15], (D_FF, D_MODEL), D_FF ** -0.5, 0.0625, ((0, 4), (1, 8)))
    return {"residual": residual, "query_major": query_major, "keys_major": keys_major, "values_major": values_major, "query_minor": query_minor, "keys_minor": keys_minor, "values_minor": values_minor, "lambda_major": lambda_major, "lambda_minor": lambda_minor, "gain_major": gain_major, "gain_minor": gain_minor, "output_major": output_major, "output_minor": output_minor, "mixer_gain": mixer_gain, "up_weight": up_weight, "down_weight": down_weight}


EPSILON = 1e-06

def to_wire(value):
    return lax.optimization_barrier(value.astype(jnp.bfloat16)).astype(jnp.float32)

def head_group(queries, key_rows, values, lambdas, scaling, head_count, key_size):
    value_size = values.shape[1] // head_count
    block_len = 512 if TOKENS % 512 == 0 else TOKENS
    key_pos = jnp.arange(TOKENS, dtype=jnp.int32)
    keys_all = key_rows.astype(jnp.float32).reshape(TOKENS, head_count, 2, key_size)
    values_all = values.astype(jnp.float32).reshape(TOKENS, head_count, value_size)

    def one_block(block_id):
        first_row = (block_id * block_len).astype(jnp.int32)
        query_block = lax.dynamic_slice_in_dim(queries, first_row, block_len, 0).astype(jnp.float32)
        query_block = query_block.reshape(block_len, head_count, 2, key_size)
        query_pos = first_row + jnp.arange(block_len, dtype=jnp.int32)
        visible = key_pos[None, :] // SEGMENT <= query_pos[:, None] // SEGMENT

        def one_head(head_id):
            query_head = lax.dynamic_index_in_dim(query_block, head_id, 1, keepdims=False)
            keys_head = lax.dynamic_index_in_dim(keys_all, head_id, 1, keepdims=False)
            values_head = lax.dynamic_index_in_dim(values_all, head_id, 1, keepdims=False)
            scores = jnp.einsum('qmd,kmd->mqk', query_head, keys_head) * key_size ** (-0.5)
            scores = jnp.where(visible[None], scores, -jnp.inf)
            peak = lax.optimization_barrier(jnp.max(scores, axis=-1, keepdims=True))
            weights = jnp.where(visible[None], jnp.exp(scores - peak), 0.0)
            totals = lax.optimization_barrier(jnp.sum(weights, axis=-1))
            sums = jnp.einsum('mqk,ke->mqe', to_wire(weights), values_head)
            lam_head = lambdas[head_id]
            output = sums[0] / totals[0][:, None] - lam_head * sums[1] / totals[1][:, None]
            output = output * lax.rsqrt(lax.optimization_barrier(jnp.mean(output * output, axis=-1, keepdims=True)) + EPSILON) * scaling
            return output.astype(jnp.bfloat16)
        per_head = lax.map(one_head, jnp.arange(head_count, dtype=jnp.int32))
        return jnp.transpose(per_head, (1, 0, 2)).reshape(block_len, head_count * value_size)
    blocks = lax.map(one_block, jnp.arange(TOKENS // block_len, dtype=jnp.int32))
    return blocks.reshape(TOKENS, head_count * value_size)

def reference(residual, query_major, keys_major, values_major, query_minor, keys_minor, values_minor, lambda_major, lambda_minor, gain_major, gain_minor, output_major, output_minor, mixer_gain, up_weight, down_weight):
    heads_major = head_group(query_major, keys_major, values_major, lambda_major, gain_major, H_MAJOR, DK_MAJOR)
    heads_minor = head_group(query_minor, keys_minor, values_minor, lambda_minor, gain_minor, H_MINOR, DK_MINOR)
    cols_major = H_MAJOR * DV_MAJOR // N_TP
    cols_minor = H_MINOR * DV_MINOR // N_TP
    mixed = jnp.zeros((TOKENS, D_MODEL), jnp.float32)
    for group in range(N_TP):
        partial_sum = jnp.dot(heads_major[:, group * cols_major:(group + 1) * cols_major], output_major[group * cols_major:(group + 1) * cols_major], preferred_element_type=jnp.float32)
        partial_sum = partial_sum + jnp.dot(heads_minor[:, group * cols_minor:(group + 1) * cols_minor], output_minor[group * cols_minor:(group + 1) * cols_minor], preferred_element_type=jnp.float32)
        mixed = mixed + to_wire(partial_sum)
    stream = residual.astype(jnp.float32) + mixed
    normed = stream * lax.rsqrt(lax.optimization_barrier(jnp.mean(stream * stream, axis=-1, keepdims=True)) + EPSILON) * mixer_gain
    normed = normed.astype(jnp.bfloat16)
    hidden = jnp.square(jax.nn.relu(jnp.dot(normed, up_weight, preferred_element_type=jnp.float32)))
    hidden = hidden.astype(jnp.bfloat16)
    cols_ff = D_FF // N_TP
    down_sum = jnp.zeros((TOKENS, D_MODEL), jnp.float32)
    for group in range(N_TP):
        partial_sum = jnp.dot(hidden[:, group * cols_ff:(group + 1) * cols_ff], down_weight[group * cols_ff:(group + 1) * cols_ff], preferred_element_type=jnp.float32)
        down_sum = down_sum + to_wire(partial_sum)
    return (stream + down_sum).astype(jnp.bfloat16)
```

```python
import functools

import jax
import jax.numpy as jnp
from jax import lax
from jax.experimental import pallas as pl
from jax.experimental.pallas import tpu as pltpu
from jax.sharding import PartitionSpec as P

DK_MAJOR = 64
DK_MINOR = 32
SEGMENT = 64
MAPS = 2

EPSILON = 1e-06
NEGATIVE = -1e30
LOG2_E = 1.4426950408889634
ANY = pl.BlockSpec(memory_space=pl.ANY)
VMEM = pl.BlockSpec(memory_space=pltpu.VMEM)
SMEM = pl.BlockSpec(memory_space=pltpu.SMEM)


def to_wire(value):
    return lax.optimization_barrier(value.astype(jnp.bfloat16)).astype(jnp.float32)


def grid_sizes(sp_count):
    y_count = 1 << ((sp_count.bit_length() - 1) // 2)
    return sp_count // y_count, y_count


class Gather:
    def __init__(self, sp_count, places, send_sem, recv_sem):
        self.z_count, self.y_count = grid_sizes(sp_count)
        own = lax.axis_index("sp")
        self.own, self.z, self.y = own, own // self.y_count, lax.rem(own, self.y_count)
        self.places, self.send_sem, self.recv_sem = places, send_sem, recv_sem
        self.copies = []

    def z_peer(self, step):
        return lax.rem(self.z + step, self.z_count) * self.y_count + self.y

    def y_peer(self, step):
        return self.z * self.y_count + lax.rem(self.y + step, self.y_count)

    def send(self, array, source, src_ref, target):
        copy = pltpu.make_async_remote_copy(
            src_ref=src_ref,
            dst_ref=self.places[array](source),
            send_sem=self.send_sem.at[array, len([c for c in self.copies if c[0] == array])],
            recv_sem=self.recv_sem.at[array, source],
            device_id={"sp": target},
            device_id_type=pl.DeviceIdType.MESH,
        )
        copy.start()
        self.copies.append((array, copy))

    def wait_block(self, array, source):
        place = self.places[array](source)
        pltpu.make_async_remote_copy(
            src_ref=place,
            dst_ref=place,
            send_sem=self.send_sem.at[array, 0],
            recv_sem=self.recv_sem.at[array, source],
            device_id={"sp": self.y_peer(1)},
            device_id_type=pl.DeviceIdType.MESH,
        ).wait_recv()

    def send_z(self, array, src_ref):
        for step in range(1, self.z_count):
            self.send(array, self.own, src_ref, self.z_peer(step))

    def send_y(self, array, src_ref):
        for step in range(1, self.y_count):
            self.send(array, self.own, src_ref, self.y_peer(step))

    def pass_on(self, array, step):
        source = self.z_peer(self.z_count - step)
        self.wait_block(array, source)
        for y_step in range(1, self.y_count):
            self.send(array, source, self.places[array](source), self.y_peer(y_step))

    def wait_y(self, array):
        for y_step in range(1, self.y_count):
            for z_step in range(self.z_count):
                z_at = lax.rem(self.z + z_step, self.z_count)
                self.wait_block(array, z_at * self.y_count + lax.rem(self.y + y_step, self.y_count))

    def finish(self):
        for _, copy in self.copies:
            copy.wait_send()


def mixer_kernel(
    sp_count,
    groups,
    q_major,
    k_major,
    v_major,
    q_minor,
    kv_minor,
    lam_major,
    lam_minor,
    gain_major,
    gain_minor,
    up_ref,
    down_ref,
    out_major,
    out_minor,
    up_all,
    down_all,
    k_major_all,
    v_major_all,
    kv_minor_all,
    qm_major,
    qm_minor,
    acc_major,
    acc_minor,
    peaks,
    totals,
    send_sem,
    recv_sem,
    local_sem,
):
    rows = q_major.shape[0]
    up_rows = up_ref.shape[0]

    def rows_of(ref, count):
        return lambda source: ref.at[pl.ds(pl.multiple_of(source * count, count), count), :]

    places = [
        rows_of(k_major_all, rows),
        rows_of(v_major_all, rows),
        rows_of(kv_minor_all, rows),
        rows_of(up_all, up_rows),
        lambda source: down_all.at[source],
    ]
    own_refs = [k_major, v_major, kv_minor, up_ref, down_ref]
    gather = Gather(sp_count, places, send_sem, recv_sem)
    own = gather.own

    barrier = pltpu.get_barrier_semaphore()
    peers = [gather.z_peer(step) for step in range(1, gather.z_count)]
    peers += [gather.y_peer(step) for step in range(1, gather.y_count)]
    for peer in peers:
        pl.semaphore_signal(
            barrier, inc=1, device_id={"sp": peer}, device_id_type=pl.DeviceIdType.MESH
        )
    pl.semaphore_wait(barrier, len(peers))

    for array in range(3):
        gather.send_z(array, own_refs[array])
    for array in range(3):
        gather.send_y(array, own_refs[array])
    for array in (3, 4):
        gather.send_z(array, own_refs[array])
    local = []
    for slot, array in enumerate((3, 4)):
        copy = pltpu.make_async_copy(own_refs[array], places[array](own), local_sem.at[slot])
        copy.start()
        local.append(copy)

    heads = []
    for group, (head_count, key_size) in enumerate(groups):
        q_ref, qm_ref = ((q_major, qm_major), (q_minor, qm_minor))[group]
        acc_ref = (acc_major, acc_minor)[group]
        value_size = acc_ref.shape[1]
        lanes = qm_ref.shape[2]
        for head in range(head_count):
            first = head * MAPS * key_size
            lane_first = first // lanes * lanes
            block = q_ref[:, lane_first : lane_first + lanes]
            lane = lax.broadcasted_iota(jnp.int32, block.shape, 1) + lane_first
            for m in range(MAPS):
                low = first + m * key_size
                keep = (lane >= low) & (lane < low + key_size)
                picked = jnp.where(keep, block.astype(jnp.float32), 0.0).astype(block.dtype)
                qm_ref[head, m * rows : (m + 1) * rows, :] = picked
            heads.append((group, head, len(heads), lane_first, lanes, value_size, key_size))

    minor_keys = q_minor.shape[1]
    minor_first = minor_keys // 128 * 128

    def fold(key_refs, value_refs, at, diagonal):
        window = pl.ds(at, rows)
        stored = (value_refs[0][window, :], value_refs[1][window, minor_first:])
        turned = [jnp.transpose(v.astype(jnp.float32)).astype(jnp.bfloat16) for v in stored]
        turned[1] = turned[1][minor_keys - minor_first :, :]
        for group, head, index, lane_first, lanes, value_size, key_size in heads:
            qm_ref = (qm_major, qm_minor)[group]
            acc_ref = (acc_major, acc_minor)[group]
            keys = key_refs[group][window, lane_first : lane_first + lanes]
            values = turned[group][head * value_size : (head + 1) * value_size, :]
            scores = lax.dot_general(
                keys, qm_ref[head], (((1,), (1,)), ((), ())), preferred_element_type=jnp.float32
            ) * (key_size ** (-0.5) * LOG2_E)
            if diagonal:
                key_pos = lax.broadcasted_iota(jnp.int32, scores.shape, 0)
                query_pos = lax.broadcasted_iota(jnp.int32, scores.shape, 1) % rows
                visible = key_pos // SEGMENT <= query_pos // SEGMENT
                scores = jnp.where(visible, scores, NEGATIVE)
            peak = jnp.max(scores, axis=0, keepdims=True)
            if not diagonal:
                peak_old = peaks[index]
                peak = jnp.maximum(peak, peak_old)
            weights = jnp.exp2(scores - peak)
            total = jnp.sum(weights, axis=0, keepdims=True)
            sums = jnp.dot(
                values, weights.astype(jnp.bfloat16), preferred_element_type=jnp.float32
            )
            if not diagonal:
                factor = jnp.exp2(peak_old - peak)
                total = total + totals[index] * factor
                sums = sums + acc_ref[head] * factor
            peaks[index] = peak
            totals[index] = total
            acc_ref[head] = sums

    fold((k_major, kv_minor), (v_major, kv_minor), 0, True)

    for step in range(1, gather.z_count):
        for array in range(3):
            gather.pass_on(array, step)
    for array in (3, 4):
        gather.send_y(array, own_refs[array])
    for array in range(3):
        gather.wait_y(array)

    def earlier(block, carry):
        at = pl.multiple_of(block * rows, rows)
        fold((k_major_all, kv_minor_all), (v_major_all, kv_minor_all), at, False)
        return carry

    lax.fori_loop(0, own, earlier, 0)

    for group, (head_count, _) in enumerate(groups):
        acc_ref = (acc_major, acc_minor)[group]
        lam_ref = (lam_major, lam_minor)[group]
        gain_ref = (gain_major, gain_minor)[group]
        out_ref = (out_major, out_minor)[group]
        done = []
        for head in range(head_count):
            index = next(h[2] for h in heads if h[0] == group and h[1] == head)
            ratio = acc_ref[head] / totals[index]
            diff = ratio[:, :rows] - lam_ref[head] * ratio[:, rows:]
            mean = jnp.mean(diff * diff, axis=0, keepdims=True)
            done.append(diff * lax.rsqrt(mean + EPSILON) * gain_ref[...])
        out_ref[...] = jnp.transpose(jnp.concatenate(done, axis=0)).astype(out_ref.dtype)

    for step in range(1, gather.z_count):
        for array in (3, 4):
            gather.pass_on(array, step)
    for array in (3, 4):
        gather.wait_y(array)
    for copy in local:
        copy.wait()
    gather.finish()


def mixer(sp_count, *args):
    q_major, k_major, v_major, q_minor, kv_minor = args[:5]
    up_weight, down_weight = args[9:11]
    heads_major = k_major.shape[1] // (MAPS * DK_MAJOR)
    heads_minor = q_minor.shape[1] // (MAPS * DK_MINOR)
    rows = q_major.shape[0]
    size_major = v_major.shape[1] // heads_major
    width_minor = kv_minor.shape[1] - q_minor.shape[1]
    size_minor = width_minor // heads_minor
    lanes_major = min(MAPS * DK_MAJOR, q_major.shape[1])
    lanes_minor = min(128, q_minor.shape[1])
    z_count, y_count = grid_sizes(sp_count)
    sends = (z_count - 1) + (y_count - 1) * z_count
    tokens = rows * sp_count
    bf16, f32 = jnp.bfloat16, jnp.float32
    head_total = heads_major + heads_minor
    return pl.pallas_call(
        functools.partial(
            mixer_kernel, sp_count, ((heads_major, DK_MAJOR), (heads_minor, DK_MINOR))
        ),
        out_shape=(
            jax.ShapeDtypeStruct(v_major.shape, bf16),
            jax.ShapeDtypeStruct((rows, width_minor), bf16),
            jax.ShapeDtypeStruct((up_weight.shape[0] * sp_count, up_weight.shape[1]), bf16),
            jax.ShapeDtypeStruct((sp_count, *down_weight.shape), bf16),
        ),
        in_specs=[VMEM] * 5 + [SMEM] * 2 + [VMEM] * 4,
        out_specs=(VMEM, VMEM, ANY, ANY),
        scratch_shapes=[
            pltpu.VMEM((tokens, k_major.shape[1]), bf16),
            pltpu.VMEM((tokens, v_major.shape[1]), bf16),
            pltpu.VMEM((tokens, kv_minor.shape[1]), bf16),
            pltpu.VMEM((heads_major, MAPS * rows, lanes_major), bf16),
            pltpu.VMEM((heads_minor, MAPS * rows, lanes_minor), bf16),
            pltpu.VMEM((heads_major, size_major, MAPS * rows), f32),
            pltpu.VMEM((heads_minor, size_minor, MAPS * rows), f32),
            pltpu.VMEM((head_total, 1, MAPS * rows), f32),
            pltpu.VMEM((head_total, 1, MAPS * rows), f32),
            pltpu.SemaphoreType.DMA((5, sends)),
            pltpu.SemaphoreType.DMA((5, sp_count)),
            pltpu.SemaphoreType.DMA((2,)),
        ],
        compiler_params=pltpu.CompilerParams(
            collective_id=0, has_side_effects=True, vmem_limit_bytes=60 * 1024 * 1024
        ),
    )(*args)


def normalize(stream, scaling):
    normed = (
        stream * lax.rsqrt(jnp.mean(stream * stream, axis=-1, keepdims=True) + EPSILON) * scaling
    )
    return normed.astype(jnp.bfloat16)


def body(
    residual,
    query_major,
    keys_major,
    values_major,
    query_minor,
    keys_minor,
    values_minor,
    lambda_major,
    lambda_minor,
    gain_major,
    gain_minor,
    output_major,
    output_minor,
    mixer_gain,
    up_weight,
    down_weight,
):
    out_major, out_minor, up_full, down_full = mixer(
        lax.axis_size("sp"),
        query_major,
        keys_major,
        values_major,
        query_minor,
        jnp.concatenate([keys_minor, values_minor], axis=1),
        lambda_major,
        lambda_minor,
        gain_major[:, None],
        gain_minor[:, None],
        up_weight,
        down_weight,
    )
    partial_sum = jnp.dot(out_major, output_major, preferred_element_type=jnp.float32)
    partial_sum = partial_sum + jnp.dot(out_minor, output_minor, preferred_element_type=jnp.float32)
    mixed = lax.psum_scatter(
        to_wire(partial_sum).astype(jnp.bfloat16), "tp", scatter_dimension=0, tiled=True
    ).astype(jnp.float32)
    stream = residual.astype(jnp.float32) + mixed
    normed_all = lax.all_gather(normalize(stream, mixer_gain), "tp", axis=0, tiled=True)
    pre_act = jnp.dot(
        normed_all,
        up_full,
        preferred_element_type=jnp.float32,
    )
    hidden = jnp.square(jax.nn.relu(pre_act)).astype(jnp.bfloat16)
    down_sum = lax.psum_scatter(
        to_wire(
            jnp.einsum("th,shd->tsd", hidden, down_full, preferred_element_type=jnp.float32)
        )
        .astype(jnp.bfloat16)
        .reshape(stream.shape[0] * lax.axis_size("tp"), -1),
        "tp",
        scatter_dimension=0,
        tiled=True,
    ).astype(jnp.float32)
    return (stream + down_sum).astype(jnp.bfloat16)


def solution(mesh):
    return jax.shard_map(
        body,
        mesh=mesh,
        in_specs=(
            P(("sp", "tp"), None),
            P("sp", "tp"),
            P("sp", "tp"),
            P("sp", "tp"),
            P("sp", "tp"),
            P("sp", "tp"),
            P("sp", "tp"),
            P("tp"),
            P("tp"),
            P(),
            P(),
            P("tp", None),
            P("tp", None),
            P(),
            P("sp", "tp"),
            P("tp", "sp"),
        ),
        out_specs=P(("sp", "tp"), None),
        check_vma=False,
    )
```

```python
import functools

import jax
import jax.numpy as jnp
from jax import lax
from jax.experimental import pallas as pl
from jax.experimental.pallas import tpu as pltpu
from jax.sharding import PartitionSpec as P

DK_MAJOR = 64
DK_MINOR = 32
SEGMENT = 64
MAPS = 2

EPSILON = 1e-06
NEGATIVE = -1e30
LOG2_E = 1.4426950408889634
ANY = pl.BlockSpec(memory_space=pl.ANY)
VMEM = pl.BlockSpec(memory_space=pltpu.VMEM)
SMEM = pl.BlockSpec(memory_space=pltpu.SMEM)


def grid_sizes(sp_count):
    y_count = 1 << ((sp_count.bit_length() - 1) // 2)
    return sp_count // y_count, y_count


class Gather:
    def __init__(self, sp_count, places, send_sem, recv_sem):
        self.z_count, self.y_count = grid_sizes(sp_count)
        own = lax.axis_index("sp")
        self.own, self.z, self.y = own, own // self.y_count, lax.rem(own, self.y_count)
        self.places, self.send_sem, self.recv_sem = places, send_sem, recv_sem
        self.copies = []

    def z_peer(self, step):
        return lax.rem(self.z + step, self.z_count) * self.y_count + self.y

    def y_peer(self, step):
        return self.z * self.y_count + lax.rem(self.y + step, self.y_count)

    def send(self, array, source, src_ref, target):
        copy = pltpu.make_async_remote_copy(
            src_ref=src_ref,
            dst_ref=self.places[array](source),
            send_sem=self.send_sem.at[array, len([c for c in self.copies if c[0] == array])],
            recv_sem=self.recv_sem.at[array, source],
            device_id={"sp": target},
            device_id_type=pl.DeviceIdType.MESH,
        )
        copy.start()
        self.copies.append((array, copy))

    def wait_block(self, array, source):
        place = self.places[array](source)
        pltpu.make_async_remote_copy(
            src_ref=place,
            dst_ref=place,
            send_sem=self.send_sem.at[array, 0],
            recv_sem=self.recv_sem.at[array, source],
            device_id={"sp": self.y_peer(1)},
            device_id_type=pl.DeviceIdType.MESH,
        ).wait_recv()

    def send_z(self, array, src_ref):
        for step in range(1, self.z_count):
            self.send(array, self.own, src_ref, self.z_peer(step))

    def send_y(self, array, src_ref):
        for step in range(1, self.y_count):
            self.send(array, self.own, src_ref, self.y_peer(step))

    def pass_on(self, array, step):
        source = self.z_peer(self.z_count - step)
        self.wait_block(array, source)
        for y_step in range(1, self.y_count):
            self.send(array, source, self.places[array](source), self.y_peer(y_step))

    def wait_y(self, array):
        for y_step in range(1, self.y_count):
            for z_step in range(self.z_count):
                z_at = lax.rem(self.z + z_step, self.z_count)
                self.wait_block(array, z_at * self.y_count + lax.rem(self.y + y_step, self.y_count))

    def finish(self):
        for _, copy in self.copies:
            copy.wait_send()


def mixer_kernel(
    sp_count,
    groups,
    q_major,
    k_major,
    v_major,
    q_minor,
    kv_minor,
    lam_major,
    lam_minor,
    gain_major,
    gain_minor,
    up_ref,
    down_ref,
    out_major,
    out_minor,
    up_all,
    down_all,
    k_major_all,
    v_major_all,
    kv_minor_all,
    qm_major,
    qm_minor,
    acc_major,
    acc_minor,
    peaks,
    totals,
    send_sem,
    recv_sem,
    local_sem,
):
    rows = q_major.shape[0]
    up_rows = up_ref.shape[0]

    def rows_of(ref, count):
        return lambda source: ref.at[pl.ds(pl.multiple_of(source * count, count), count), :]

    places = [
        rows_of(k_major_all, rows),
        rows_of(v_major_all, rows),
        rows_of(kv_minor_all, rows),
        rows_of(up_all, up_rows),
        lambda source: down_all.at[source],
    ]
    own_refs = [k_major, v_major, kv_minor, up_ref, down_ref]
    gather = Gather(sp_count, places, send_sem, recv_sem)
    own = gather.own

    barrier = pltpu.get_barrier_semaphore()
    peers = [gather.z_peer(step) for step in range(1, gather.z_count)]
    peers += [gather.y_peer(step) for step in range(1, gather.y_count)]
    for peer in peers:
        pl.semaphore_signal(
            barrier, inc=1, device_id={"sp": peer}, device_id_type=pl.DeviceIdType.MESH
        )
    pl.semaphore_wait(barrier, len(peers))

    for array in range(3):
        gather.send_z(array, own_refs[array])
    for array in range(3):
        gather.send_y(array, own_refs[array])
    for array in (3, 4):
        gather.send_z(array, own_refs[array])
    for array in (3, 4):
        gather.send_y(array, own_refs[array])
    local = []
    for slot, array in enumerate((3, 4)):
        copy = pltpu.make_async_copy(own_refs[array], places[array](own), local_sem.at[slot])
        copy.start()
        local.append(copy)

    heads = []
    for group, (head_count, key_size) in enumerate(groups):
        q_ref, qm_ref = ((q_major, qm_major), (q_minor, qm_minor))[group]
        acc_ref = (acc_major, acc_minor)[group]
        value_size = acc_ref.shape[1]
        lanes = qm_ref.shape[2]
        for head in range(head_count):
            first = head * MAPS * key_size
            lane_first = first // lanes * lanes
            block = q_ref[:, lane_first : lane_first + lanes]
            lane = lax.broadcasted_iota(jnp.int32, block.shape, 1) + lane_first
            for m in range(MAPS):
                low = first + m * key_size
                keep = (lane >= low) & (lane < low + key_size)
                picked = jnp.where(keep, block.astype(jnp.float32), 0.0).astype(block.dtype)
                qm_ref[head, m * rows : (m + 1) * rows, :] = picked
            heads.append((group, head, len(heads), lane_first, lanes, value_size, key_size))

    minor_keys = q_minor.shape[1]
    minor_first = minor_keys // 128 * 128

    def fold(key_refs, value_refs, at, diagonal):
        window = pl.ds(at, rows)
        stored = (value_refs[0][window, :], value_refs[1][window, minor_first:])
        turned = [jnp.transpose(v.astype(jnp.float32)).astype(jnp.bfloat16) for v in stored]
        turned[1] = turned[1][minor_keys - minor_first :, :]
        for group, head, index, lane_first, lanes, value_size, key_size in heads:
            qm_ref = (qm_major, qm_minor)[group]
            acc_ref = (acc_major, acc_minor)[group]
            keys = key_refs[group][window, lane_first : lane_first + lanes]
            values = turned[group][head * value_size : (head + 1) * value_size, :]
            scores = lax.dot_general(
                keys, qm_ref[head], (((1,), (1,)), ((), ())), preferred_element_type=jnp.float32
            ) * (key_size ** (-0.5) * LOG2_E)
            if diagonal:
                key_pos = lax.broadcasted_iota(jnp.int32, scores.shape, 0)
                query_pos = lax.broadcasted_iota(jnp.int32, scores.shape, 1) % rows
                visible = key_pos // SEGMENT <= query_pos // SEGMENT
                scores = jnp.where(visible, scores, NEGATIVE)
            peak = jnp.max(scores, axis=0, keepdims=True)
            if not diagonal:
                peak_old = peaks[index]
                peak = jnp.maximum(peak, peak_old)
            weights = jnp.exp2(scores - peak)
            total = jnp.sum(weights, axis=0, keepdims=True)
            sums = jnp.dot(
                values, weights.astype(jnp.bfloat16), preferred_element_type=jnp.float32
            )
            if not diagonal:
                factor = jnp.exp2(peak_old - peak)
                total = total + totals[index] * factor
                sums = sums + acc_ref[head] * factor
            peaks[index] = peak
            totals[index] = total
            acc_ref[head] = sums

    fold((k_major, kv_minor), (v_major, kv_minor), 0, True)

    for step in range(1, gather.z_count):
        for array in range(3):
            gather.pass_on(array, step)

    def earlier(block, carry):
        at = pl.multiple_of(block * rows, rows)
        fold((k_major_all, kv_minor_all), (v_major_all, kv_minor_all), at, False)
        return carry

    y_count = gather.y_count

    def same_y(z_at, carry):
        return earlier(z_at * y_count + gather.y, carry)

    def other_y(index, carry):
        z_at, place = index // (y_count - 1), lax.rem(index, y_count - 1)
        y_at = place + (place >= gather.y).astype(jnp.int32)
        return earlier(z_at * y_count + y_at, carry)

    lax.fori_loop(0, gather.z, same_y, 0)
    for array in range(3):
        gather.wait_y(array)
    lax.fori_loop(0, gather.z * (y_count - 1) + gather.y, other_y, 0)

    for group, (head_count, _) in enumerate(groups):
        acc_ref = (acc_major, acc_minor)[group]
        lam_ref = (lam_major, lam_minor)[group]
        gain_ref = (gain_major, gain_minor)[group]
        out_ref = (out_major, out_minor)[group]
        done = []
        for head in range(head_count):
            index = next(h[2] for h in heads if h[0] == group and h[1] == head)
            ratio = acc_ref[head] / totals[index]
            diff = ratio[:, :rows] - lam_ref[head] * ratio[:, rows:]
            mean = jnp.mean(diff * diff, axis=0, keepdims=True)
            done.append(diff * lax.rsqrt(mean + EPSILON) * gain_ref[...])
        out_ref[...] = jnp.transpose(jnp.concatenate(done, axis=0)).astype(out_ref.dtype)

    for step in range(1, gather.z_count):
        for array in (3, 4):
            gather.pass_on(array, step)
    for array in (3, 4):
        gather.wait_y(array)
    for copy in local:
        copy.wait()
    gather.finish()


def mixer(sp_count, *args):
    q_major, k_major, v_major, q_minor, kv_minor = args[:5]
    up_weight, down_weight = args[9:11]
    heads_major = k_major.shape[1] // (MAPS * DK_MAJOR)
    heads_minor = q_minor.shape[1] // (MAPS * DK_MINOR)
    rows = q_major.shape[0]
    size_major = v_major.shape[1] // heads_major
    width_minor = kv_minor.shape[1] - q_minor.shape[1]
    size_minor = width_minor // heads_minor
    lanes_major = min(MAPS * DK_MAJOR, q_major.shape[1])
    lanes_minor = min(128, q_minor.shape[1])
    z_count, y_count = grid_sizes(sp_count)
    sends = (z_count - 1) + (y_count - 1) * z_count
    tokens = rows * sp_count
    bf16, f32 = jnp.bfloat16, jnp.float32
    head_total = heads_major + heads_minor
    return pl.pallas_call(
        functools.partial(
            mixer_kernel, sp_count, ((heads_major, DK_MAJOR), (heads_minor, DK_MINOR))
        ),
        out_shape=(
            jax.ShapeDtypeStruct(v_major.shape, bf16),
            jax.ShapeDtypeStruct((rows, width_minor), bf16),
            jax.ShapeDtypeStruct((up_weight.shape[0] * sp_count, up_weight.shape[1]), bf16),
            jax.ShapeDtypeStruct((sp_count, *down_weight.shape), bf16),
        ),
        in_specs=[VMEM] * 5 + [SMEM] * 2 + [VMEM] * 4,
        out_specs=(VMEM, VMEM, ANY, ANY),
        scratch_shapes=[
            pltpu.VMEM((tokens, k_major.shape[1]), bf16),
            pltpu.VMEM((tokens, v_major.shape[1]), bf16),
            pltpu.VMEM((tokens, kv_minor.shape[1]), bf16),
            pltpu.VMEM((heads_major, MAPS * rows, lanes_major), bf16),
            pltpu.VMEM((heads_minor, MAPS * rows, lanes_minor), bf16),
            pltpu.VMEM((heads_major, size_major, MAPS * rows), f32),
            pltpu.VMEM((heads_minor, size_minor, MAPS * rows), f32),
            pltpu.VMEM((head_total, 1, MAPS * rows), f32),
            pltpu.VMEM((head_total, 1, MAPS * rows), f32),
            pltpu.SemaphoreType.DMA((5, sends)),
            pltpu.SemaphoreType.DMA((5, sp_count)),
            pltpu.SemaphoreType.DMA((2,)),
        ],
        compiler_params=pltpu.CompilerParams(
            collective_id=0, has_side_effects=True, vmem_limit_bytes=60 * 1024 * 1024
        ),
    )(*args)


class Exchange:
    def __init__(self, tp_count, send_sem, recv_sem):
        own = lax.axis_index("tp")
        self.x_count = tp_count // 2
        self.own, self.x, self.core = own, own // 2, lax.rem(own, 2)
        self.partner = self.x * 2 + 1 - self.core
        self.send_sem, self.recv_sem = send_sem, recv_sem

    def enter(self):
        barrier = pltpu.get_barrier_semaphore()
        peers = [self.partner] + [self.x_peer(step) for step in range(1, self.x_count)]
        for peer in peers:
            pl.semaphore_signal(
                barrier, inc=1, device_id={"tp": peer}, device_id_type=pl.DeviceIdType.MESH
            )
        pl.semaphore_wait(barrier, len(peers))

    def x_peer(self, step):
        return lax.rem(self.x + step, self.x_count) * 2 + self.core

    def copy(self, src, dst, slot, target):
        made = pltpu.make_async_remote_copy(
            src_ref=src,
            dst_ref=dst,
            send_sem=self.send_sem.at[slot],
            recv_sem=self.recv_sem.at[slot],
            device_id={"tp": target},
            device_id_type=pl.DeviceIdType.MESH,
        )
        made.start()
        return made

    def total(self, partial, pair_in, pair_sum, x_in, rows):
        def block(x_at, core):
            return pl.ds(pl.multiple_of((x_at * 2 + core) * rows, rows), rows)

        steps = list(range(1, self.x_count)) + [0]
        at = [lax.rem(self.x + step, self.x_count) for step in range(self.x_count)]
        pair = {}
        for step in steps:
            pair[step] = self.copy(
                partial.at[block(at[step], 1 - self.core), :], pair_in.at[step], step, self.partner
            )
        across = []
        for step in steps:
            pair[step].wait_recv()
            mine = partial[block(at[step], self.core), :].astype(jnp.float32)
            both = mine + pair_in[step].astype(jnp.float32)
            if step:
                pair_sum[step] = both.astype(jnp.bfloat16)
                across.append(
                    self.copy(
                        pair_sum.at[step], x_in.at[step], self.x_count + step, self.x_peer(step)
                    )
                )
        for made in across:
            made.wait_recv()
        for step in range(1, self.x_count):
            both = both + x_in[step].astype(jnp.float32)
        return both, list(pair.values()) + across


def mix_kernel(
    tp_count, partial, residual, gain, stream_ref, normed_ref, pair_in, pair_sum, x_in, held, send_sem, recv_sem
):
    exchange = Exchange(tp_count, send_sem, recv_sem)
    exchange.enter()
    rows = residual.shape[0]
    mixed, copies = exchange.total(partial, pair_in, pair_sum, x_in, rows)
    stream = residual[...].astype(jnp.float32) + mixed
    stream_ref[...] = stream
    mean = jnp.mean(stream * stream, axis=-1, keepdims=True)
    normed = (stream * lax.rsqrt(mean + EPSILON) * gain[...]).astype(jnp.bfloat16)
    held[...] = normed

    def place(index):
        return normed_ref.at[pl.ds(pl.multiple_of(index * rows, rows), rows), :]

    base, count = 2 * exchange.x_count, exchange.x_count
    sent = [exchange.copy(held, place(exchange.own), base + step, exchange.x_peer(step)) for step in range(1, count)]
    passed = [exchange.copy(held, place(exchange.own), base + count, exchange.partner)]
    normed_ref[pl.ds(pl.multiple_of(exchange.own * rows, rows), rows), :] = normed
    for step in range(1, count):
        sent[step - 1].wait_recv()
        source = exchange.x_peer(count - step)
        passed.append(
            exchange.copy(place(source), place(source), base + count + step, exchange.partner)
        )
    for made in passed:
        made.wait_recv()
    for made in copies + sent + passed:
        made.wait_send()


def sum_kernel(tp_count, partial, stream, out_ref, pair_in, pair_sum, x_in, send_sem, recv_sem):
    exchange = Exchange(tp_count, send_sem, recv_sem)
    exchange.enter()
    total, copies = exchange.total(partial, pair_in, pair_sum, x_in, stream.shape[0])
    out_ref[...] = (stream[...] + total).astype(out_ref.dtype)
    for made in copies:
        made.wait_send()


def tp_call(kernel, identity, inputs, out_shape, rows, holds):
    tp_count = lax.axis_size("tp")
    slots = (tp_count // 2, rows, inputs[0].shape[1])
    held = [pltpu.VMEM(slots[1:], jnp.bfloat16)] if holds else []
    return pl.pallas_call(
        functools.partial(kernel, tp_count),
        out_shape=out_shape,
        in_specs=[VMEM] * len(inputs),
        out_specs=jax.tree.map(lambda _: VMEM, out_shape),
        scratch_shapes=[pltpu.VMEM(slots, jnp.bfloat16)] * 3
        + held
        + [pltpu.SemaphoreType.DMA((2 * tp_count,))] * 2,
        compiler_params=pltpu.CompilerParams(
            collective_id=identity, has_side_effects=True, vmem_limit_bytes=32 * 1024 * 1024
        ),
    )(*inputs)


def body(
    residual,
    query_major,
    keys_major,
    values_major,
    query_minor,
    keys_minor,
    values_minor,
    lambda_major,
    lambda_minor,
    gain_major,
    gain_minor,
    output_major,
    output_minor,
    mixer_gain,
    up_weight,
    down_weight,
):
    out_major, out_minor, up_full, down_full = mixer(
        lax.axis_size("sp"),
        query_major,
        keys_major,
        values_major,
        query_minor,
        jnp.concatenate([keys_minor, values_minor], axis=1),
        lambda_major,
        lambda_minor,
        gain_major[:, None],
        gain_minor[:, None],
        up_weight,
        down_weight,
    )
    partial_sum = jnp.dot(out_major, output_major, preferred_element_type=jnp.float32)
    partial_sum = partial_sum + jnp.dot(out_minor, output_minor, preferred_element_type=jnp.float32)
    rows = residual.shape[0]
    stream, normed_all = tp_call(
        mix_kernel,
        1,
        (partial_sum.astype(jnp.bfloat16), residual, mixer_gain[None, :]),
        (
            jax.ShapeDtypeStruct(residual.shape, jnp.float32),
            jax.ShapeDtypeStruct(partial_sum.shape, jnp.bfloat16),
        ),
        rows,
        True,
    )
    pre_act = jnp.dot(
        normed_all,
        up_full,
        preferred_element_type=jnp.float32,
    )
    hidden = jnp.square(jax.nn.relu(pre_act)).astype(jnp.bfloat16)
    down_part = jnp.einsum("th,shd->tsd", hidden, down_full, preferred_element_type=jnp.float32)
    down_part = down_part.astype(jnp.bfloat16).reshape(partial_sum.shape)
    return tp_call(
        sum_kernel,
        2,
        (down_part, stream),
        jax.ShapeDtypeStruct(residual.shape, residual.dtype),
        rows,
        False,
    )


def solution(mesh):
    return jax.shard_map(
        body,
        mesh=mesh,
        in_specs=(
            P(("sp", "tp"), None),
            P("sp", "tp"),
            P("sp", "tp"),
            P("sp", "tp"),
            P("sp", "tp"),
            P("sp", "tp"),
            P("sp", "tp"),
            P("tp"),
            P("tp"),
            P(),
            P(),
            P("tp", None),
            P("tp", None),
            P(),
            P("sp", "tp"),
            P("tp", "sp"),
        ),
        out_specs=P(("sp", "tp"), None),
        check_vma=False,
    )
```
